32 devices in a mesh: sp: 4 (over z), tp: 2 (over y), dp: 4 (over x, core).
Axes of the slice: x: 2, y: 2, z: 4, core: 2. Of those that a mesh axis runs over, the one named last changes fastest.
Arguments:
- latents: bfloat16 [4, 2048, 3072], P('dp', ('sp', 'tp')), may hold values from -5 to 5
- condition: bfloat16 [4, 3072], P('dp', ('sp', 'tp')), may hold values from -6 to 6
- context: bfloat16 [4, 384, 3072], P('dp', ('sp', 'tp')), may hold values from -6 to 6
- context_cond: bfloat16 [3072], P(('sp', 'tp')), may hold values from -6 to 6
- shift_weight: bfloat16 [3072, 3072], P(('sp', 'tp')), may hold values from -0.109375 to 0.109375
- scale_weight: bfloat16 [3072, 3072], P(('sp', 'tp')), may hold values from -0.109375 to 0.109375
- out_gate_weight: bfloat16 [3072, 3072], P(('sp', 'tp')), may hold values from -0.109375 to 0.109375
- pre_gain: float32 [3072], replicated, may hold values from 0.1 to 1.9
- post_gain: float32 [3072], replicated, may hold values from 0.1 to 1.9
- query_weight: bfloat16 [3072, 1024], P(None, 'tp'), may hold values from -0.108253175 to 0.108253175
- key_weight: bfloat16 [3072, 256], replicated, may hold values from -0.108253175 to 0.108253175
- value_weight: bfloat16 [3072, 256], replicated, may hold values from -0.109375 to 0.109375
- head_gate_weight: bfloat16 [3072, 1024], P(None, 'tp'), may hold values from -0.109375 to 0.109375
- lambdas: float32 [8], P('tp'), may hold values from 0.3 to 0.8
- head_gain: float32 [128], replicated, may hold values from 0.1 to 1.9
- out_weight: bfloat16 [1024, 3072], P(None, 'tp'), may hold values from -0.1875 to 0.1875
Outputs:
- mixed_out: bfloat16 [4, 2048, 3072], P('dp', ('sp', 'tp'))
The draws below stay inside these ranges and needn't reach their ends.
All inputs are finite; a program needn't handle non-finite values.
Results may differ from the reference program's by a relative error of at most 0.0128.
The reference program's roundings to bfloat16 on the way (of `silu_cond`, `silu_context`, `latent_in`, `context_in`, `weights`, `branch` and `projected`) count: a program that leaves them out, or rounds other values in their place, can miss the bound.
Values may be sent and summed in bfloat16 or wider, within the bound.
A program may use at most 64 MiB of HBM per device.

```python
import jax
import jax.numpy as jnp
from jax import lax

D = 3072
HEADS = 8
KVH = 2
HQK = 64
HV = 128
CTX = 384
SAMPLES = 4
LAT = 2048


def draw_latents(key, part):
    values = jnp.clip(jax.random.normal(jax.random.fold_in(key, 21), (SAMPLES, LAT, D), jnp.float32), -5.0, 5.0)
    return values.astype(jnp.bfloat16)


def draw_query_weight(key, part):
    values = jnp.clip(jax.random.normal(jax.random.fold_in(key, 31), (D, HEADS * 2 * HQK), jnp.float32), -5.0, 5.0) * D ** (-0.5)
    return values.astype(jnp.bfloat16)


def draw_key_weight(key, part):
    values = jnp.clip(jax.random.normal(jax.random.fold_in(key, 41), (D, KVH * 2 * HQK), jnp.float32), -5.0, 5.0) * D ** (-0.5)
    return values.astype(jnp.bfloat16)


def shard_levels(rng, shape, shards, least, high):
    factor_of, own = 1.0, jax.random.fold_in(rng, 6)
    for dim, shards_of in shards:
        heights = jnp.exp(jax.random.uniform(jax.random.fold_in(own, dim), (shards_of,), jnp.float32, least / len(shards), high / len(shards)))
        factor_of = factor_of * jnp.repeat(heights, shape[dim] // shards_of).reshape([-1 if axis == dim else 1 for axis in range(len(shape))])
    return factor_of


def noise(own_key, extent, scale, most, cuts=(), held_as=jnp.bfloat16):
    drawn = scale * jax.random.normal(own_key, extent, jnp.float32)
    if cuts:
        drawn = drawn * shard_levels(own_key, extent, cuts, -0.22, 0.18)
    return jnp.clip(drawn, -most, most).astype(held_as)


def setup_inputs(seed: int = 0) -> dict:
    key_of = jax.random.split(jax.random.key(seed), 17)
    return {
        "latents": draw_latents(jax.random.fold_in(key_of[16], 71), 0),
        "condition": noise(key_of[1], (SAMPLES, D), 1.0, 6.0, ((0, 4), (1, 8))),
        "context": noise(key_of[2], (SAMPLES, CTX, D), 1.0, 6.0, ((0, 4), (1, 8))),
        "context_cond": noise(key_of[3], (D,), 1.0, 6.0, ((0, 8),)),
        "shift_weight": noise(key_of[4], (D, D), D ** -0.5, 0.109375, ((0, 8),)),
        "scale_weight": noise(key_of[5], (D, D), D ** -0.5, 0.109375, ((0, 8),)),
        "out_gate_weight": noise(key_of[6], (D, D), D ** -0.5, 0.109375, ((0, 8),)),
        "pre_gain": jnp.clip(1.0 + 0.18 * jax.random.normal(key_of[7], (D,), jnp.float32), 0.1, 1.9),
        "post_gain": jnp.clip(1.0 + 0.18 * jax.random.normal(key_of[8], (D,), jnp.float32), 0.1, 1.9),
        "query_weight": draw_query_weight(jax.random.fold_in(key_of[16], 71), 0),
        "key_weight": draw_key_weight(jax.random.fold_in(key_of[16], 71), 0),
        "value_weight": noise(key_of[11], (D, KVH * HV), D ** -0.5, 0.109375),
        "head_gate_weight": noise(key_of[12], (D, HEADS * HV), D ** -0.5, 0.109375, ((1, 2),)),
        "lambdas": jnp.clip(0.3 + 0.5 * jax.random.uniform(key_of[13], (HEADS,), jnp.float32) ** shard_levels(key_of[13], (HEADS,), ((0, 2),), -0.2, 0.2), 0.3, 0.8),
        "head_gain": jnp.clip(1.0 + 0.18 * jax.random.normal(key_of[14], (HV,), jnp.float32), 0.1, 1.9),
        "out_weight": noise(key_of[15], (HEADS * HV, D), (HEADS * HV) ** -0.5, 0.1875, ((1, 2),)),
    }


NORM_EPSILON = 1e-06

def norm_rows(values, norm_gain):
    return values * lax.rsqrt(lax.optimization_barrier(jnp.mean(values * values, axis=-1, keepdims=True)) + NORM_EPSILON) * norm_gain

def rounded(values):
    return lax.optimization_barrier(values.astype(jnp.bfloat16))

def project(tokens, weight):
    flattened = tokens.reshape(-1, tokens.shape[-1])
    result = jnp.dot(flattened, weight, preferred_element_type=jnp.float32)
    return rounded(result).reshape(tokens.shape[:-1] + (weight.shape[1],))

def reference(latents, condition, context, context_cond, shift_weight, scale_weight, out_gate_weight, pre_gain, post_gain, query_weight, key_weight, value_weight, head_gate_weight, lambdas, head_gain, out_weight):
    silu_cond = rounded(jax.nn.silu(condition.astype(jnp.float32)))
    silu_context = rounded(jax.nn.silu(context_cond.astype(jnp.float32)))[None, :]
    shifts = jnp.dot(silu_cond, shift_weight, preferred_element_type=jnp.float32)
    scales = jnp.dot(silu_cond, scale_weight, preferred_element_type=jnp.float32)
    out_gate = jnp.dot(silu_cond, out_gate_weight, preferred_element_type=jnp.float32)
    context_shift = jnp.dot(silu_context, shift_weight, preferred_element_type=jnp.float32)
    context_scale = jnp.dot(silu_context, scale_weight, preferred_element_type=jnp.float32)
    latent_in = rounded(norm_rows(latents.astype(jnp.float32), pre_gain) * (1.0 + scales[:, None, :]) + shifts[:, None, :])
    context_in = rounded(norm_rows(context.astype(jnp.float32), pre_gain) * (1.0 + context_scale[:, None, :]) + context_shift[:, None, :])
    queries = project(latent_in, query_weight).reshape(SAMPLES, LAT, HEADS, 2, HQK)
    head_gate = project(latent_in, head_gate_weight).reshape(SAMPLES, LAT, HEADS, HV)
    joined = jnp.concatenate([context_in, latent_in], axis=1)
    key_rows = project(joined, key_weight).reshape(SAMPLES, CTX + LAT, KVH, 2, HQK)
    value_rows = project(joined, value_weight).reshape(SAMPLES, CTX + LAT, KVH, HV)
    group_size = HEADS // KVH

    def one_head(item_index):
        sample_index = item_index // HEADS
        head_index = item_index % HEADS
        key_group = head_index // group_size
        one_query = queries[sample_index, :, head_index].astype(jnp.float32)
        one_key = key_rows[sample_index, :, key_group].astype(jnp.float32)
        one_value = value_rows[sample_index, :, key_group].astype(jnp.float32)
        scores = jnp.einsum('qmd,kmd->mqk', one_query, one_key) * HQK ** (-0.5)
        largest = lax.optimization_barrier(jnp.max(scores, axis=-1, keepdims=True))
        exponent = jnp.exp(scores - largest)
        normalizer = lax.optimization_barrier(jnp.sum(exponent, axis=-1))
        weights = rounded(exponent).astype(jnp.float32)
        weighted = jnp.einsum('mqk,kv->mqv', weights, one_value)
        ratios = weighted / normalizer[..., None]
        attended = ratios[0] - lambdas[head_index] * ratios[1]
        gate_input = head_gate[sample_index, :, head_index].astype(jnp.float32)
        return rounded(norm_rows(attended, head_gain) * jax.nn.silu(gate_input))
    branch = lax.map(one_head, jnp.arange(SAMPLES * HEADS, dtype=jnp.int32))
    branch = branch.reshape(SAMPLES, HEADS, LAT, HV).transpose(0, 2, 1, 3).reshape(SAMPLES, LAT, HEADS * HV)
    projected = project(branch, out_weight)
    mixed_out = out_gate[:, None, :] * norm_rows(projected.astype(jnp.float32), post_gain)
    return mixed_out.astype(jnp.bfloat16)
```

```python
import functools
import math

import jax
import jax.numpy as jnp
from jax import lax
from jax.experimental import pallas as pl
from jax.experimental.pallas import tpu as pltpu
from jax.sharding import PartitionSpec as P

HEADS = 8
KVH = 2
HQK = 64
HV = 128
NORM_EPSILON = 1e-06
MESH = pl.DeviceIdType.MESH
SUBLANES = 16
LANES = 128


def norm_rows(values, norm_gain):
    return (
        values
        * lax.rsqrt(jnp.mean(values * values, axis=-1, keepdims=True) + NORM_EPSILON)
        * norm_gain
    )


def shifted(values, axis, size, step):
    return lax.ppermute(values, axis, [(i, (i + step) % size) for i in range(size)])


def each(count, body):
    if count <= 8:
        for index in range(count):
            body(index)
    else:
        pl.loop(0, count)(body)


def only(always, condition, body):
    if always:
        body()
    else:
        pl.when(condition)(body)


def flip(index, bit):
    return index + bit - 2 * bit * lax.rem(index // bit, 2)


def lanes(start, size):
    return pl.ds(pl.multiple_of(start, LANES), size)


def rows_at(start, size):
    return pl.ds(pl.multiple_of(start, math.gcd(size, SUBLANES)), size)


class Plan:
    def __init__(self, sp, tp, dp, rows, context, model, weight_shape, query_columns):
        self.sp, self.tp, self.dp = sp, tp, dp
        self.group = sp * tp
        self.rows, self.context, self.model = rows, context, model
        self.local_heads = query_columns // (2 * HQK)
        self.per_group = (HEADS // KVH) // self.local_heads
        self.padded = -(-(rows + context) // SUBLANES) * SUBLANES
        self.owners = math.gcd(model // LANES, self.group)
        self.slice = model // self.owners
        self.depth, self.columns = weight_shape
        self.quarter = self.depth // dp
        self.pair = math.gcd(math.gcd(sp, 2), self.quarter // SUBLANES)
        self.share = self.quarter // self.pair
        quarter_rows = max(SUBLANES, rows // 4 // SUBLANES * SUBLANES)
        cuts = list(range(0, rows, quarter_rows))
        self.chunks = [(start, min(quarter_rows, rows - start)) for start in cuts]


def modulate_rows(source, target, start, count, target_start, gain_scale, shift):
    block = math.gcd(count, 32)

    def step(index):
        offset = pl.multiple_of(index * block, block)
        values = source[pl.ds(start + offset, block), :].astype(jnp.float32)
        factor = lax.rsqrt(jnp.mean(values * values, axis=-1, keepdims=True) + NORM_EPSILON)
        result = values * factor * gain_scale + shift
        target[pl.ds(target_start + offset, block), :] = result.astype(jnp.bfloat16)

    pl.loop(0, count // block)(step)


def project_rows(source, start, count, weight, target, target_start):
    columns = weight.shape[1]
    width = math.gcd(columns, 256)

    def step(index):
        at = lanes(index * width, width)
        target[pl.ds(target_start, count), at] = jnp.dot(
            source[pl.ds(start, count), :], weight[:, at], preferred_element_type=jnp.float32
        ).astype(jnp.bfloat16)

    pl.loop(0, columns // width)(step)


def front_kernel(
    plan,
    cond_ref, context_cond_ref, gain_ref,
    latents, context, shift_weight, scale_weight, gate_weight,
    query_weight, key_weight, value_weight, head_gate_weight, out_weight,
    q_ref, g_ref, kv_ref, wo_ref, sums_ref,
    wcond, own_rows, own_context, own_in, kv_weight, q_weight, g_weight,
    other_rows, other_in, kv_made, parts, held,
    load_sem, sum_send, sum_recv, all_send, all_recv,
    row_send, row_recv, kvy_send, kvy_recv, kvz_send, kvz_recv,
    wy_send, wy_recv, wz_send, wz_recv, wd_send, wd_recv,
):
    sp, tp, dp, group = plan.sp, plan.tp, plan.dp, plan.group
    s, t, d = lax.axis_index("sp"), lax.axis_index("tp"), lax.axis_index("dp")
    me = s * tp + t
    rows, context_rows = plan.rows, plan.context

    def load(index, source, target):
        copy = pltpu.make_async_copy(source, target, load_sem.at[index])
        copy.start()
        return copy

    cond_loads = [
        load(i, w, wcond.at[i]) for i, w in enumerate((shift_weight, scale_weight, gate_weight))
    ]
    row_load = load(3, latents, own_rows)
    context_load = load(4, context, own_context)
    kv_loads = []
    for head in range(KVH):
        for part, weight in enumerate((key_weight, value_weight)):
            kv_loads.append(
                load(
                    5 + 2 * head + part,
                    weight.at[:, pl.ds(head * LANES, LANES)],
                    kv_weight.at[:, pl.ds((2 * head + part) * LANES, LANES)],
                )
            )
    late_loads = [
        load(5 + 2 * KVH, query_weight, q_weight),
        load(6 + 2 * KVH, head_gate_weight, g_weight),
    ]

    def member(offset):
        other = lax.rem(me + offset, group)
        return {"sp": other // tp, "tp": lax.rem(other, tp)}

    def remote(source, target, send, recv, device):
        return pltpu.make_async_remote_copy(
            src_ref=source, dst_ref=target, send_sem=send, recv_sem=recv,
            device_id=device, device_id_type=MESH,
        )

    bits = []
    bit = dp // 2
    while bit:
        bits.append(bit)
        bit //= 2

    barrier = pltpu.get_barrier_semaphore()

    def greet(index):
        pl.semaphore_signal(
            barrier, inc=1, device_id=member(index + 1), device_id_type=MESH
        )

    each(group - 1, greet)
    for bit in bits:
        pl.semaphore_signal(
            barrier, inc=1, device_id={"dp": flip(d, bit)}, device_id_type=MESH
        )
    pl.semaphore_wait(barrier, group - 1 + len(bits))

    base = s - lax.rem(s, plan.pair)

    def weight_rows(ring):
        return rows_at((d * plan.pair + ring) * plan.share, plan.share)

    def over_tp(step):
        return {"tp": lax.rem(t + step, tp)}

    def weight_y(step):
        ring = lax.rem(s, plan.pair)
        return remote(
            out_weight.at[weight_rows(ring), :],
            wo_ref.at[step - 1, weight_rows(ring), :],
            wy_send.at[step - 1], wy_recv.at[step - 1], over_tp(step),
        )

    def weight_z(step, turn):
        ring = lax.rem(s, plan.pair)
        return remote(
            wo_ref.at[step - 1, weight_rows(ring), :],
            wo_ref.at[step - 1, weight_rows(ring), :],
            wz_send.at[step - 1, turn - 1], wz_recv.at[step - 1, turn - 1],
            {"sp": base + lax.rem(ring + turn, plan.pair)},
        )

    def weight_d(step, level, index):
        bit = bits[level]
        turns = [0]
        for earlier in bits[:level]:
            turns += [turn ^ earlier for turn in turns]
        source = d
        for other in bits:
            if turns[index] & other:
                source = flip(source, other)
        at = rows_at(source * plan.quarter, plan.quarter)
        slot = (2**level - 1) + index
        return remote(
            wo_ref.at[step - 1, at, :], wo_ref.at[step - 1, at, :],
            wd_send.at[step - 1, slot], wd_recv.at[step - 1, slot],
            {"dp": flip(d, bit)},
        )

    def row_copy(step, chunk):
        start, count = plan.chunks[chunk]
        return remote(
            latents.at[pl.ds(start, count), :],
            other_rows.at[step - 1, pl.ds(start, count), :],
            row_send.at[step - 1, chunk], row_recv.at[step - 1, chunk], over_tp(step),
        )

    for step in range(1, tp):
        weight_y(step).start()

    conditions = []
    for ref in (cond_ref, context_cond_ref):
        value = ref[...].astype(jnp.float32)
        conditions.append(value / (1.0 + jnp.exp(-value)))
    depth = cond_ref.shape[1]
    index = lax.broadcasted_iota(jnp.int32, (8, depth), 0)
    first = jnp.broadcast_to(conditions[0], (8, depth))
    second = jnp.broadcast_to(conditions[1], (8, depth))
    total = None
    for copy in cond_loads:
        copy.wait()
    lefts = []
    for number in range(3):
        left = jnp.where(index == 2 * number, first, 0.0)
        if number < 2:
            left = jnp.where(index == 2 * number + 1, second, left)
        lefts.append(left.astype(jnp.bfloat16))
    width = plan.slice

    def partial_sums(column):
        at = lanes(column * width, width)
        total = None
        for number in range(3):
            part = jnp.dot(
                lefts[number], wcond[number, :, at], preferred_element_type=jnp.float32
            )
            total = part if total is None else total + part
        parts[:, at] = total

    each(plan.owners, partial_sums)

    every = plan.owners == group

    def scatter(index):
        owner = lax.rem(me + index + 1, group)
        return remote(
            parts.at[:, lanes(lax.rem(owner, plan.owners) * width, width)],
            held.at[index], sum_send.at[index], sum_recv.at[index], member(index + 1),
        ), owner < plan.owners

    def scatter_start(index):
        copy, valid = scatter(index)
        only(every, valid, copy.start)

    each(group - 1, scatter_start)
    for step in range(1, tp):
        row_copy(step, 0).start()

    own_slice = lanes(lax.rem(me, plan.owners) * width, width)

    def gather(index):
        return remote(
            sums_ref.at[:, own_slice], sums_ref.at[:, own_slice],
            all_send.at[index], all_recv.at[index], member(index + 1),
        )

    def arrived(index):
        origin = lax.rem(me + group - index - 1, group)
        at = lanes(lax.rem(origin, plan.owners) * width, width)
        return remote(
            sums_ref.at[:, at], sums_ref.at[:, at],
            all_send.at[index], all_recv.at[index], member(index + 1),
        ), origin < plan.owners

    def own_sum():
        each(group - 1, lambda index: scatter(index)[0].wait_recv())
        total = parts[:, own_slice]
        if group <= 16:
            for index in range(group - 1):
                total = total + held[index]
        else:
            total = lax.fori_loop(
                0, group - 1, lambda index, value: value + held[index], total
            )
        sums_ref[:, own_slice] = total
        each(group - 1, lambda index: gather(index).start())

    only(every, me < plan.owners, own_sum)

    for step in range(1, tp):
        weight_y(step).wait_recv()
        for turn in range(1, plan.pair):
            weight_z(step, turn).start()
    row_load.wait()
    context_load.wait()

    def sum_arrival(index):
        copy, valid = arrived(index)
        only(every, valid, copy.wait_recv)

    each(group - 1, sum_arrival)
    gain = gain_ref[...]
    shift, context_shift = sums_ref[0:1, :], sums_ref[1:2, :]
    scale, context_scale = 1.0 + sums_ref[2:3, :], 1.0 + sums_ref[3:4, :]
    modulate_rows(own_rows, own_in, 0, rows, 0, gain * scale, shift)
    values = own_context[...].astype(jnp.float32)
    factor = lax.rsqrt(jnp.mean(values * values, axis=-1, keepdims=True) + NORM_EPSILON)
    values = (values * factor * (gain * context_scale) + context_shift)
    fill = plan.padded - rows - context_rows
    if fill:
        values = jnp.concatenate([values, jnp.zeros((fill, values.shape[1]), values.dtype)], axis=0)
    own_in[rows:, :] = values.astype(jnp.bfloat16)
    for copy in kv_loads:
        copy.wait()

    def make_kv(head):
        kv_made[head] = jnp.dot(
            own_in[...], kv_weight[:, lanes(head * 2 * LANES, 2 * LANES)],
            preferred_element_type=jnp.float32,
        ).astype(jnp.bfloat16)

    pl.loop(0, KVH)(make_kv)

    def kv_group(index):
        return index // plan.per_group

    def kv_y(step):
        return remote(
            kv_made.at[kv_group(lax.rem(t + step, tp))], kv_ref.at[me],
            kvy_send.at[step - 1], kvy_recv.at[step - 1], over_tp(step),
        )

    def kv_y_arrival(step):
        block = s * tp + lax.rem(t + tp - step, tp)
        return remote(
            kv_made.at[0], kv_ref.at[block],
            kvy_send.at[step - 1], kvy_recv.at[step - 1], over_tp(step),
        )

    def over_sp(index):
        return {"sp": lax.rem(s + index + 1, sp)}

    def kv_z(step, index):
        block = s * tp + lax.rem(t + tp - step, tp)
        source = kv_made.at[kv_group(t)] if step == 0 else kv_ref.at[block]
        return remote(
            source, kv_ref.at[block],
            kvz_send.at[step, index], kvz_recv.at[step, index], over_sp(index),
        )

    for step in range(1, tp):
        kv_y(step).start()
    own_block = pltpu.make_async_copy(
        kv_made.at[kv_group(t)], kv_ref.at[me], load_sem.at[7 + 2 * KVH]
    )
    own_block.start()
    each(sp - 1, lambda index: kv_z(0, index).start())
    for step in range(1, tp):
        for chunk in range(1, len(plan.chunks)):
            row_copy(step, chunk).start()

    for step in range(1, tp):
        for turn in range(1, plan.pair):
            weight_z(step, turn).wait_recv()
        if bits:
            weight_d(step, 0, 0).start()

    for copy in late_loads:
        copy.wait()
    project_rows(own_in, 0, rows, q_weight, q_ref, 0)
    project_rows(own_in, 0, rows, g_weight, g_ref, 0)

    for step in range(1, tp):
        kv_y_arrival(step).wait_recv()
        each(sp - 1, lambda index, step=step: kv_z(step, index).start())

    for level in range(len(bits)):
        if level + 1 == len(bits):
            break
        for step in range(1, tp):
            for index in range(2**level):
                weight_d(step, level, index).wait_recv()
            for index in range(2 ** (level + 1)):
                weight_d(step, level + 1, index).start()

    gain_scale = gain * scale
    for chunk in range(len(plan.chunks)):
        start, count = plan.chunks[chunk]
        for step in range(1, tp):
            row_copy(step, chunk).wait_recv()
            modulate_rows(other_rows.at[step - 1], other_in, start, count, 0, gain_scale, shift)
            project_rows(other_in, 0, count, q_weight, q_ref, step * rows + start)
            project_rows(other_in, 0, count, g_weight, g_ref, step * rows + start)

    for step in range(tp):
        each(sp - 1, lambda index, step=step: kv_z(step, index).wait_recv())
    own_block.wait()
    if bits:
        level = len(bits) - 1
        for step in range(1, tp):
            for index in range(2**level):
                weight_d(step, level, index).wait_recv()

    def scatter_done(index):
        copy, valid = scatter(index)
        only(every, valid, copy.wait_send)

    each(group - 1, scatter_done)
    only(
        every, me < plan.owners,
        lambda: each(group - 1, lambda index: gather(index).wait_send()),
    )
    for step in range(1, tp):
        weight_y(step).wait_send()
        kv_y(step).wait_send()
        for turn in range(1, plan.pair):
            weight_z(step, turn).wait_send()
        for chunk in range(len(plan.chunks)):
            row_copy(step, chunk).wait_send()
        for level in range(len(bits)):
            for index in range(2**level):
                weight_d(step, level, index).wait_send()
    for step in range(tp):
        each(sp - 1, lambda index, step=step: kv_z(step, index).wait_send())


def front(plan, small, large):
    sp, tp, dp, group = plan.sp, plan.tp, plan.dp, plan.group
    rows, model = plan.rows, plan.model
    columns = plan.local_heads * 2 * HQK
    largest = max(count for _, count in plan.chunks)
    others = tp - 1
    turns = max(plan.pair - 1, 1)
    swaps = max(dp - 1, 1)
    bf16, f32 = jnp.bfloat16, jnp.float32
    vmem = pl.BlockSpec(memory_space=pltpu.VMEM)
    dma = pltpu.SemaphoreType.DMA
    condition = small[0].shape[1]
    return pl.pallas_call(
        functools.partial(front_kernel, plan),
        out_shape=(
            jax.ShapeDtypeStruct((tp * rows, columns), bf16),
            jax.ShapeDtypeStruct((tp * rows, columns), bf16),
            jax.ShapeDtypeStruct((group, plan.padded, 2 * LANES), bf16),
            jax.ShapeDtypeStruct((others, plan.depth, plan.columns), bf16),
            jax.ShapeDtypeStruct((8, model), f32),
        ),
        in_specs=[vmem] * len(small) + [pl.BlockSpec(memory_space=pl.ANY)] * len(large),
        out_specs=(vmem,) * 5,
        scratch_shapes=[
            pltpu.VMEM((3, condition, model), bf16),
            pltpu.VMEM((rows, model), bf16),
            pltpu.VMEM((plan.context, model), bf16),
            pltpu.VMEM((plan.padded, model), bf16),
            pltpu.VMEM((model, KVH * 2 * LANES), bf16),
            pltpu.VMEM((model, columns), bf16),
            pltpu.VMEM((model, columns), bf16),
            pltpu.VMEM((others, rows, model), bf16),
            pltpu.VMEM((largest, model), bf16),
            pltpu.VMEM((KVH, plan.padded, 2 * LANES), bf16),
            pltpu.VMEM((8, model), f32),
            pltpu.VMEM((group - 1, 8, plan.slice), f32),
            dma((8 + 2 * KVH,)),
            dma((group - 1,)), dma((group - 1,)), dma((group - 1,)), dma((group - 1,)),
            dma((others, len(plan.chunks))), dma((others, len(plan.chunks))),
            dma((others,)), dma((others,)),
            dma((tp, sp - 1)), dma((tp, sp - 1)),
            dma((others,)), dma((others,)),
            dma((others, turns)), dma((others, turns)),
            dma((others, swaps)), dma((others, swaps)),
        ],
        compiler_params=pltpu.CompilerParams(
            collective_id=0, has_side_effects=True, vmem_limit_bytes=60 * 2**20
        ),
        cost_estimate=pl.CostEstimate(
            flops=2 * (tp * rows + plan.padded) * model * 2 * columns,
            bytes_accessed=30 * 10**6, transcendentals=0,
        ),
    )(*small, *large)


def attend_kernel(used, lambda_ref, q_ref, gate_ref, gain_ref, k_ref, v_ref, out_ref):
    queries = q_ref[...]
    rows = queries.shape[0]
    lane = lax.broadcasted_iota(jnp.int32, queries.shape, 1)
    queries = queries.astype(jnp.float32) * HQK ** (-0.5)
    both = jnp.concatenate(
        [jnp.where(lane < HQK, queries, 0.0), jnp.where(lane < HQK, 0.0, queries)], axis=0
    ).astype(jnp.bfloat16)
    contract = (((1,), (1,)), ((), ()))
    blocks, size, width = k_ref.shape
    keys = k_ref[...].reshape(blocks * size, width)
    values = v_ref[...].reshape(blocks * size, width)
    scores = lax.dot_general(both, keys, contract, preferred_element_type=jnp.float32)
    if used < size:
        column = lax.broadcasted_iota(jnp.int32, scores.shape, 1)
        scores = jnp.where(lax.rem(column, size) < used, scores, -jnp.inf)
    largest = jnp.max(scores, axis=-1, keepdims=True)
    exponent = jnp.exp(scores - largest)
    normalizer = jnp.sum(exponent, axis=-1, keepdims=True)
    weighted = jnp.dot(exponent.astype(jnp.bfloat16), values, preferred_element_type=jnp.float32)
    ratios = weighted / normalizer
    attended = ratios[:rows] - lambda_ref[pl.program_id(0)] * ratios[rows:]
    gate = jax.nn.silu(gate_ref[...].astype(jnp.float32))
    out_ref[...] = (norm_rows(attended, gain_ref[...]) * gate).astype(jnp.bfloat16)


def attend(plan, lambdas, queries, gate, head_gain, kv, first, count):
    heads = plan.local_heads
    block = math.gcd(count, 128)
    skip = first // block
    blocks, size, _ = kv.shape
    tile = pl.BlockSpec((block, 128), lambda h, i: (i + skip, h))
    return pl.pallas_call(
        functools.partial(attend_kernel, plan.rows + plan.context),
        grid=(heads, count // block),
        out_shape=jax.ShapeDtypeStruct((count, heads * HV), jnp.bfloat16),
        in_specs=[
            pl.BlockSpec(memory_space=pltpu.SMEM),
            tile,
            tile,
            pl.BlockSpec((1, HV), lambda h, i: (0, 0)),
            pl.BlockSpec((blocks, size, 128), lambda h, i: (0, 0, 0)),
            pl.BlockSpec((blocks, size, 128), lambda h, i: (0, 0, 1)),
        ],
        out_specs=pl.BlockSpec((block, 128), lambda h, i: (i, h)),
        compiler_params=pltpu.CompilerParams(vmem_limit_bytes=48 * 2**20),
        cost_estimate=pl.CostEstimate(
            flops=16 * heads * count * blocks * size * HV, bytes_accessed=4 * 10**6,
            transcendentals=2 * heads * count * blocks * size,
        ),
    )(lambdas, queries, gate, head_gain, kv, kv)


def tail_kernel(tp, *refs):
    branches, refs = refs[:tp], refs[tp:]
    own_weight, other_weight, sums_ref, gain_ref, out_ref, branch, projected = refs
    me = lax.axis_index("tp")
    width = branches[0].shape[1]
    columns = own_weight.shape[1]
    for step in range(tp):
        owner = lax.rem(me + step, tp)
        branch[:, pl.ds(pl.multiple_of(owner * width, width), width)] = branches[step][...]
    projected[:, pl.ds(pl.multiple_of(me * columns, columns), columns)] = jnp.dot(
        branch[...], own_weight[...], preferred_element_type=jnp.float32
    )
    for step in range(1, tp):
        owner = lax.rem(me - step + tp, tp)
        projected[:, pl.ds(pl.multiple_of(owner * columns, columns), columns)] = jnp.dot(
            branch[...], other_weight[step - 1], preferred_element_type=jnp.float32
        )
    values = projected[...].astype(jnp.bfloat16).astype(jnp.float32)
    out_ref[...] = (sums_ref[4:5, :] * norm_rows(values, gain_ref[...])).astype(jnp.bfloat16)


def tail(branches, own_weight, other_weight, sums, post_gain, tp):
    rows = branches[0].shape[0]
    width = post_gain.shape[1]
    operands = (*branches, own_weight, other_weight, sums, post_gain)
    return pl.pallas_call(
        functools.partial(tail_kernel, tp),
        out_shape=jax.ShapeDtypeStruct((rows, width), jnp.bfloat16),
        in_specs=[pl.BlockSpec(memory_space=pltpu.VMEM)] * len(operands),
        out_specs=pl.BlockSpec(memory_space=pltpu.VMEM),
        scratch_shapes=[
            pltpu.VMEM((rows, own_weight.shape[0]), jnp.bfloat16),
            pltpu.VMEM((rows, width), jnp.float32),
        ],
        compiler_params=pltpu.CompilerParams(vmem_limit_bytes=48 * 2**20),
        cost_estimate=pl.CostEstimate(
            flops=2 * rows * width * own_weight.shape[0], bytes_accessed=10**7, transcendentals=0
        ),
    )(*operands)


def local(
    sp, tp, dp,
    latents, condition, context, context_cond,
    shift_weight, scale_weight, out_gate_weight,
    pre_gain, post_gain,
    query_weight, key_weight, value_weight, head_gate_weight,
    lambdas, head_gain, out_weight,
):
    rows = latents.shape[1]
    plan = Plan(
        sp, tp, dp, rows, context.shape[1], latents.shape[2],
        out_weight.shape, query_weight.shape[1],
    )
    queries, gate, kv, other_weight, sums = front(
        plan,
        (condition, context_cond[None, :], pre_gain[None, :]),
        (
            latents[0], context[0], shift_weight, scale_weight, out_gate_weight,
            query_weight, key_weight, value_weight, head_gate_weight, out_weight,
        ),
    )
    gain = head_gain[None, :]
    other_branch = attend(plan, lambdas, queries, gate, gain, kv, rows, (tp - 1) * rows)
    returned = [
        shifted(other_branch[(step - 1) * rows : step * rows], "tp", tp, tp - step)
        for step in range(1, tp)
    ]
    own_branch = attend(plan, lambdas, queries, gate, gain, kv, 0, rows)
    result = tail(
        [own_branch, *returned], out_weight, other_weight, sums, post_gain[None, :], tp
    )
    return result[None]


def solution(mesh):
    return jax.shard_map(
        functools.partial(local, mesh.shape["sp"], mesh.shape["tp"], mesh.shape["dp"]),
        mesh=mesh,
        in_specs=(
            P("dp", ("sp", "tp"), None),
            P("dp", ("sp", "tp")),
            P("dp", ("sp", "tp"), None),
            P(("sp", "tp")),
            P(("sp", "tp"), None),
            P(("sp", "tp"), None),
            P(("sp", "tp"), None),
            P(),
            P(),
            P(None, "tp"),
            P(),
            P(),
            P(None, "tp"),
            P("tp"),
            P(),
            P(None, "tp"),
        ),
        out_specs=P("dp", ("sp", "tp"), None),
        check_vma=False,
    )
```

```python
import functools
import math

import jax
import jax.numpy as jnp
from jax import lax
from jax.experimental import pallas as pl
from jax.experimental.pallas import tpu as pltpu
from jax.sharding import PartitionSpec as P

HEADS = 8
KVH = 2
HQK = 64
HV = 128
NORM_EPSILON = 1e-06
MESH = pl.DeviceIdType.MESH
SUBLANES = 16
LANES = 128


def norm_rows(values):
    return values * lax.rsqrt(jnp.mean(values * values, axis=-1, keepdims=True) + NORM_EPSILON)


def each(count, body):
    if count <= 8:
        for index in range(count):
            body(index)
    else:
        pl.loop(0, count)(body)


def only(always, condition, body):
    if always:
        body()
    else:
        pl.when(condition)(body)


def flip(index, bit):
    return index + bit - 2 * bit * lax.rem(index // bit, 2)


def lanes(start, size):
    return pl.ds(pl.multiple_of(start, LANES), size)


def rows_at(start, size):
    return pl.ds(pl.multiple_of(start, math.gcd(size, SUBLANES)), size)


class Plan:
    def __init__(self, sp, tp, dp, rows, context, model, weight_shape, query_columns):
        self.sp, self.tp, self.dp = sp, tp, dp
        self.group = sp * tp
        self.rows, self.context, self.model = rows, context, model
        self.columns = query_columns
        self.local_heads = query_columns // (2 * HQK)
        self.per_group = (HEADS // KVH) // self.local_heads
        self.used = rows + context
        self.padded = -(-self.used // SUBLANES) * SUBLANES
        self.owners = math.gcd(model // LANES, self.group)
        self.slice = model // self.owners
        self.depth, self.out_columns = weight_shape
        self.quarter = self.depth // dp
        self.pair = math.gcd(math.gcd(sp, 2), self.quarter // SUBLANES)
        self.share = self.quarter // self.pair
        self.parts = math.gcd(4, self.share // SUBLANES)
        self.unit = max(SUBLANES, rows // 4 // SUBLANES * SUBLANES)
        self.units = rows // self.unit
        self.stack = self.local_heads * 2 * self.unit
        self.half = self.stack // 2
        self.halves = 2 if self.unit % (2 * SUBLANES) == 0 else 1
        self.near = (tp + sp - 1) * self.padded
        self.far = (tp - 1) * (sp - 1) * self.padded
        self.groups = [[0]] + [[chunk] for chunk in range(1, self.units)]
        if self.units > 2:
            self.groups = [[0, 1]] + [[chunk] for chunk in range(2, self.units)]


def modulate_rows(source, target, start, count, target_start, gain_scale, shift):
    block = math.gcd(count, 32)

    def step(index):
        offset = pl.multiple_of(index * block, block)
        values = norm_rows(source[pl.ds(start + offset, block), :].astype(jnp.float32))
        result = values * gain_scale + shift
        target[pl.ds(target_start + offset, block), :] = result.astype(jnp.bfloat16)

    pl.loop(0, count // block)(step)


def mega_kernel(
    plan,
    lambda_ref, cond_ref, context_cond_ref, gain_ref, post_gain_ref, head_gain_ref,
    latents, context, shift_weight, scale_weight, gate_weight,
    query_weight, key_weight, value_weight, head_gate_weight, out_weight,
    out_ref,
    wcond, own_rows, own_context, own_in, kv_weight, q_weight, g_weight, own_out_weight,
    other_out_weight, other_rows, other_in, kv_made, kv, parts, held, sums, normed,
    queries, gates, scores_a, scores_b, weighted, normalizer, largest, branch, back, projected,
    load_sem, sum_send, sum_recv, all_send, all_recv,
    row_send, row_recv, kvy_send, kvy_recv, kvz_send, kvz_recv,
    wy_send, wy_recv, wz_send, wz_recv, wx_send, wx_recv, wd_send, wd_recv,
    back_send, back_recv,
):
    sp, tp, dp, group = plan.sp, plan.tp, plan.dp, plan.group
    s, t, d = lax.axis_index("sp"), lax.axis_index("tp"), lax.axis_index("dp")
    me = s * tp + t
    rows, context_rows, unit, units = plan.rows, plan.context, plan.unit, plan.units
    heads, columns, size = plan.local_heads, plan.columns, plan.padded
    f32, bf16 = jnp.float32, jnp.bfloat16

    def load(index, source, target):
        copy = pltpu.make_async_copy(source, target, load_sem.at[index])
        copy.start()
        return copy

    cond_loads = [
        load(i, w, wcond.at[i]) for i, w in enumerate((shift_weight, scale_weight, gate_weight))
    ]
    row_load = load(3, latents, own_rows)
    context_load = load(4, context, own_context)
    def member(offset):
        other = lax.rem(me + offset, group)
        return {"sp": other // tp, "tp": lax.rem(other, tp)}

    def remote(source, target, send, recv, device):
        return pltpu.make_async_remote_copy(
            src_ref=source, dst_ref=target, send_sem=send, recv_sem=recv,
            device_id=device, device_id_type=MESH,
        )

    bits = []
    bit = dp // 2
    while bit:
        bits.append(bit)
        bit //= 2

    barrier = pltpu.get_barrier_semaphore()

    def greet(index):
        pl.semaphore_signal(
            barrier, inc=1, device_id=member(index + 1), device_id_type=MESH
        )

    each(group - 1, greet)
    for bit in bits:
        pl.semaphore_signal(
            barrier, inc=1, device_id={"dp": flip(d, bit)}, device_id_type=MESH
        )

    base = s - lax.rem(s, plan.pair)
    ring = lax.rem(s, plan.pair)
    piece = plan.share // plan.parts

    def over_tp(step):
        return {"tp": lax.rem(t + step, tp)}

    def weight_y(step, part):
        at = rows_at((d * plan.pair + ring) * plan.share + part * piece, piece)
        return remote(
            out_weight.at[at, :], other_out_weight.at[step - 1, at, :],
            wy_send.at[step - 1, part], wy_recv.at[step - 1, part], over_tp(step),
        )

    def weight_z(step, turn, part):
        at = rows_at((d * plan.pair + ring) * plan.share + part * piece, piece)
        return remote(
            other_out_weight.at[step - 1, at, :], other_out_weight.at[step - 1, at, :],
            wz_send.at[step - 1, turn - 1, part], wz_recv.at[step - 1, turn - 1, part],
            {"sp": base + lax.rem(ring + turn, plan.pair)},
        )

    def weight_x(step, turn, part):
        source = lax.rem(ring + turn, plan.pair)
        at = rows_at((d * plan.pair + source) * plan.share + part * piece, piece)
        return remote(
            other_out_weight.at[step - 1, at, :], other_out_weight.at[step - 1, at, :],
            wx_send.at[step - 1, turn, part], wx_recv.at[step - 1, turn, part],
            {"dp": flip(d, bits[0])},
        )

    def weight_d(step, level, index):
        turns = [0]
        for earlier in bits[:level]:
            turns += [turn ^ earlier for turn in turns]
        source = d
        for other in bits:
            if turns[index] & other:
                source = flip(source, other)
        at = rows_at(source * plan.quarter, plan.quarter)
        slot = (2**level - 1) + index
        return remote(
            other_out_weight.at[step - 1, at, :], other_out_weight.at[step - 1, at, :],
            wd_send.at[step - 1, slot], wd_recv.at[step - 1, slot],
            {"dp": flip(d, bits[level])},
        )

    def level_copies(step, level):
        if level == 0:
            return [
                weight_x(step, turn, part)
                for turn in range(plan.pair) for part in range(plan.parts)
            ]
        return [weight_d(step, level, index) for index in range(2**level)]

    def row_copy(step, chunk):
        at = pl.ds(chunk * unit, unit)
        return remote(
            latents.at[at, :], other_rows.at[step - 1, at, :],
            row_send.at[step - 1, chunk], row_recv.at[step - 1, chunk], over_tp(step),
        )

    def over_tp_steps(body):
        for step in range(1, tp):
            body(step)

    with jax.named_scope("enter"):
        pl.semaphore_wait(barrier, group - 1 + len(bits))

    def weight_start(part):
        if part < plan.parts:
            over_tp_steps(lambda step: weight_y(step, part).start())

    def weight_forward(part):
        if part < plan.parts:
            for step in range(1, tp):
                weight_y(step, part).wait_recv()
                if bits:
                    weight_x(step, 0, part).start()
                for turn in range(1, plan.pair):
                    weight_z(step, turn, part).start()

    weight_start(0)

    with jax.named_scope("conditions"):
        conditions = []
        for ref in (cond_ref, context_cond_ref):
            value = ref[...].astype(f32)
            conditions.append(value / (1.0 + jnp.exp(-value)))
        depth = cond_ref.shape[1]
        index = lax.broadcasted_iota(jnp.int32, (8, depth), 0)
        first = jnp.broadcast_to(conditions[0], (8, depth))
        second = jnp.broadcast_to(conditions[1], (8, depth))
        lefts = []
        for number in range(3):
            left = jnp.where(index == 2 * number, first, 0.0)
            if number < 2:
                left = jnp.where(index == 2 * number + 1, second, left)
            lefts.append(left.astype(bf16))
        width = plan.slice
        for copy in cond_loads:
            copy.wait()
        kv_loads = []
        for head in range(KVH):
            for part, weight in enumerate((key_weight, value_weight)):
                kv_loads.append(
                    load(
                        5 + 2 * head + part,
                        weight.at[:, pl.ds(head * LANES, LANES)],
                        kv_weight.at[:, pl.ds((2 * head + part) * LANES, LANES)],
                    )
                )
        late_loads = [
            load(5 + 2 * KVH, query_weight, q_weight),
            load(6 + 2 * KVH, head_gate_weight, g_weight),
        ]
        tail_load = load(7 + 2 * KVH, out_weight, own_out_weight)

        def partial_sums(column):
            at = lanes(column * width, width)
            total = None
            for number in range(3):
                part = jnp.dot(lefts[number], wcond[number, :, at], preferred_element_type=f32)
                total = part if total is None else total + part
            parts[:, at] = total

        each(plan.owners, partial_sums)

    every = plan.owners == group

    def scatter(index):
        owner = lax.rem(me + index + 1, group)
        return remote(
            parts.at[:, lanes(lax.rem(owner, plan.owners) * width, width)],
            held.at[index], sum_send.at[index], sum_recv.at[index], member(index + 1),
        ), owner < plan.owners

    def scatter_start(index):
        copy, valid = scatter(index)
        only(every, valid, copy.start)

    each(group - 1, scatter_start)

    weight_start(1)
    row_load.wait()
    block = math.gcd(rows, 32)

    def normalize(index):
        at = pl.ds(pl.multiple_of(index * block, block), block)
        normed[at, :] = norm_rows(own_rows[at, :].astype(f32))

    with jax.named_scope("normalize"):
        pl.loop(0, rows // block)(normalize)
        context_load.wait()
        normed[rows : rows + context_rows, :] = norm_rows(own_context[...].astype(f32))

    own_slice = lanes(lax.rem(me, plan.owners) * width, width)

    def gather(index):
        return remote(
            sums.at[:, own_slice], sums.at[:, own_slice],
            all_send.at[index], all_recv.at[index], member(index + 1),
        )

    def arrived(index):
        origin = lax.rem(me + group - index - 1, group)
        at = lanes(lax.rem(origin, plan.owners) * width, width)
        return remote(
            sums.at[:, at], sums.at[:, at],
            all_send.at[index], all_recv.at[index], member(index + 1),
        ), origin < plan.owners

    def own_sum():
        each(group - 1, lambda index: scatter(index)[0].wait_recv())
        total = parts[:, own_slice]
        if group <= 16:
            for index in range(group - 1):
                total = total + held[index]
        else:
            total = lax.fori_loop(
                0, group - 1, lambda index, value: value + held[index], total
            )
        sums[:, own_slice] = total
        each(group - 1, lambda index: gather(index).start())

    with jax.named_scope("reduce"):
        only(every, me < plan.owners, own_sum)

    weight_start(2)
    weight_start(3)
    kv[:, 2 * LANES :] = jnp.ones((kv.shape[0], LANES), bf16)

    def sum_arrival(index):
        copy, valid = arrived(index)
        only(every, valid, copy.wait_recv)

    with jax.named_scope("gather"):
        each(group - 1, sum_arrival)
    gain = gain_ref[...]
    shift, context_shift = sums[0:1, :], sums[1:2, :]
    gain_scale, context_gain_scale = gain * (1.0 + sums[2:3, :]), gain * (1.0 + sums[3:4, :])
    with jax.named_scope("modulate"):

        def modulate(index):
            at = pl.ds(pl.multiple_of(index * block, block), block)
            own_in[at, :] = (normed[at, :] * gain_scale + shift).astype(bf16)

        pl.loop(0, rows // block)(modulate)
        values = normed[rows : rows + context_rows, :] * context_gain_scale + context_shift
        if size > plan.used:
            fill = jnp.zeros((size - plan.used, plan.model), f32)
            values = jnp.concatenate([values, fill], axis=0)
        own_in[rows:, :] = values.astype(bf16)
    for copy in kv_loads:
        copy.wait()

    def make_kv(head):
        kv_made[head] = jnp.dot(
            own_in[...], kv_weight[:, lanes(head * 2 * LANES, 2 * LANES)],
            preferred_element_type=f32,
        ).astype(bf16)

    with jax.named_scope("make_kv"):
        pl.loop(0, KVH)(make_kv)

    def kv_slot(step, offset):
        slot = step if offset == 0 else tp + step * (sp - 1) + offset - 1
        return kv.at[pl.ds(slot * size, size), pl.ds(0, 2 * LANES)]

    def kv_group(column):
        return column // plan.per_group

    def kv_y(step):
        return remote(
            kv_made.at[kv_group(lax.rem(t + step, tp))], kv_slot(step, 0),
            kvy_send.at[step - 1], kvy_recv.at[step - 1], over_tp(step),
        )

    def kv_z(step, offset):
        source = kv_made.at[kv_group(t)] if step == 0 else kv_slot(step, 0)
        return remote(
            source, kv_slot(step, offset),
            kvz_send.at[step, offset - 1], kvz_recv.at[step, offset - 1],
            {"sp": lax.rem(s + offset, sp)},
        )

    over_tp_steps(lambda step: kv_y(step).start())
    own_block = load(8 + 2 * KVH, kv_made.at[kv_group(t)], kv_slot(0, 0))
    for offset in range(1, sp):
        kv_z(0, offset).start()
    for chunk in range(units):
        over_tp_steps(lambda step, chunk=chunk: row_copy(step, chunk).start())

    def project_rows(source, start, count, first_unit):
        wide = math.gcd(columns, 512)

        def make_queries(index):
            result = jnp.dot(
                source[pl.ds(start, count), :], q_weight[:, lanes(index * wide, wide)],
                preferred_element_type=f32,
            ).astype(bf16).astype(f32) * HQK ** (-0.5)
            lane = lax.broadcasted_iota(jnp.int32, (count, LANES), 1)
            for local in range(wide // LANES):
                value = result[:, local * LANES : (local + 1) * LANES]
                head = index * (wide // LANES) + local
                for number in range(2):
                    half = jnp.where((lane < HQK) == (number == 0), value, 0.0).astype(bf16)
                    for block in range(count // unit):
                        at = rows_at((head * 2 + number) * unit, unit)
                        queries[first_unit + block, at, :] = half[
                            block * unit : (block + 1) * unit
                        ]

        def make_gates(index):
            at = lanes(index * wide, wide)
            result = jnp.dot(
                source[pl.ds(start, count), :], g_weight[:, at], preferred_element_type=f32
            ).astype(bf16)
            for block in range(count // unit):
                gates[first_unit + block, :, at] = result[block * unit : (block + 1) * unit]

        pl.loop(0, columns // wide)(make_queries)
        pl.loop(0, columns // wide)(make_gates)

    for copy in late_loads:
        copy.wait()
    with jax.named_scope("own_project"):
        project_rows(own_in, 0, rows, 0)

    with jax.named_scope("kv_over_tp"):
        for step in range(1, tp):
            kv_y(step).wait_recv()
            for offset in range(1, sp):
                kv_z(step, offset).start()

    with jax.named_scope("weight_forward"):
        for part in range(plan.parts):
            weight_forward(part)

    def weight_pair_done():
        with jax.named_scope("weight_pair"):
            for step in range(1, tp):
                for turn in range(1, plan.pair):
                    for part in range(plan.parts):
                        weight_z(step, turn, part).wait_recv()
                        if bits:
                            weight_x(step, turn, part).start()

    contract = (((1,), (1,)), ((), ()))

    spans = ((0, plan.near), (plan.near, plan.far))

    def score(buffer, index, side, phase):
        begin, count = spans[phase]
        result = lax.dot_general(
            queries[index, pl.ds(side * plan.half, plan.half), :],
            kv[pl.ds(begin, count), pl.ds(0, LANES)],
            contract, preferred_element_type=f32,
        )
        if plan.used < size:
            column = lax.broadcasted_iota(jnp.int32, result.shape, 1)
            result = jnp.where(lax.rem(column, size) < plan.used, result, -jnp.inf)
        buffer[:, pl.ds(0, count)] = result

    def gather_values(buffer, index, side, phase):
        begin, count = spans[phase]
        at = pl.ds(side * plan.half, plan.half)
        scores = buffer[:, pl.ds(0, count)]
        top = jnp.max(scores, axis=-1, keepdims=True)
        if phase:
            before = largest[index, at, pl.ds(0, 1)]
            top = jnp.maximum(top, before)
        both = jnp.dot(
            jnp.exp(scores - top).astype(bf16), kv[pl.ds(begin, count), pl.ds(LANES, 2 * LANES)],
            preferred_element_type=f32,
        )
        if phase:
            keep = jnp.exp(before - top)
            weighted[index, at, :] = weighted[index, at, :] * keep + both[:, :LANES]
            normalizer[index, at, :] = normalizer[index, at, :] * keep + both[:, LANES:]
        else:
            weighted[index, at, :] = both[:, :LANES]
            normalizer[index, at, :] = both[:, LANES:]
            largest[index, at, :] = jnp.broadcast_to(top, (plan.half, LANES))

    def attend(first_unit, count, phase):
        if not spans[phase][1]:
            return
        score(scores_a, first_unit, 0, phase)

        def step(index):
            here = first_unit + index
            score(scores_b, here, 1, phase)
            gather_values(scores_a, here, 0, phase)
            score(scores_a, here + 1, 0, phase)
            gather_values(scores_b, here, 1, phase)

        if count > 1:
            pl.loop(0, count - 1)(step)
        score(scores_b, first_unit + count - 1, 1, phase)
        gather_values(scores_a, first_unit + count - 1, 0, phase)
        gather_values(scores_b, first_unit + count - 1, 1, phase)

    def finish(index, target):
        for head in range(heads):
            ratios = []
            for number in range(2):
                at = pl.ds((head * 2 + number) * unit, unit)
                ratios.append(weighted[index, at, :] / normalizer[index, at, :])
            attended = ratios[0] - lambda_ref[head] * ratios[1]
            gate = gates[index, :, pl.ds(head * LANES, LANES)].astype(f32)
            gate = gate / (1.0 + jnp.exp(-gate))
            target(head, (norm_rows(attended) * head_gain_ref[...] * gate).astype(bf16))

    def finish_own(index):
        at = rows_at(index * unit, unit)

        def store(head, value):
            branch[at, lanes(t * columns + head * LANES, LANES)] = value

        finish(index, store)

    def returned(step, chunk):
        at = pl.ds(chunk * unit, unit)
        return remote(
            back.at[step - 1, at, :], branch.at[at, lanes(t * columns, columns)],
            back_send.at[step - 1, chunk], back_recv.at[step - 1, chunk],
            over_tp(tp - step),
        )

    def returned_here(step, chunk):
        owner = lax.rem(t + step, tp)
        at = pl.ds(chunk * unit, unit)
        return remote(
            back.at[step - 1, at, :], branch.at[at, lanes(owner * columns, columns)],
            back_send.at[step - 1, chunk], back_recv.at[step - 1, chunk],
            over_tp(tp - step),
        )

    def finish_other(step, chunk):
        def store(head, value):
            back[step - 1, pl.ds(chunk * unit, unit), pl.ds(head * LANES, LANES)] = value

        finish(step * units + chunk, store)
        returned(step, chunk).start()

    def receive(chunks):
        begin, count = chunks[0] * unit, len(chunks) * unit
        for step in range(1, tp):
            with jax.named_scope("row_wait"):
                for chunk in chunks:
                    row_copy(step, chunk).wait_recv()
            with jax.named_scope("other_project"):
                modulate_rows(other_rows.at[step - 1], other_in, begin, count, 0, gain_scale, shift)
                project_rows(other_in, 0, count, step * units + chunks[0])

    def attend_other(chunks, phase):
        for step in range(1, tp):
            attend(step * units + chunks[0], len(chunks), phase)

    def kv_wait(step):
        with jax.named_scope("kv_wait"):
            for offset in range(1, sp):
                kv_z(step, offset).wait_recv()

    own_block.wait()
    kv_wait(0)
    with jax.named_scope("own_near"):
        attend(0, units, 0)
    for number, chunks in enumerate(plan.groups[:-1]):
        receive(chunks)
        with jax.named_scope("other_near"):
            attend_other(chunks, 0)
        if number == 0:
            weight_pair_done()
    if len(plan.groups) == 1:
        weight_pair_done()
    def weight_levels():
        for level in range(len(bits) - 1):
            with jax.named_scope("weight_dp"):
                for step in range(1, tp):
                    for copy in level_copies(step, level):
                        copy.wait_recv()
                    for copy in level_copies(step, level + 1):
                        copy.start()

    for step in range(1, tp):
        kv_wait(step)
    early = [chunk for chunks in plan.groups[:-1] for chunk in chunks]
    if early:
        with jax.named_scope("other_far"):
            attend_other(early, 1)
            for step in range(1, tp):
                for chunk in early:
                    finish_other(step, chunk)
    with jax.named_scope("own_far"):
        attend(0, units, 1)
        pl.loop(0, units)(finish_own)
    weight_levels()
    receive(plan.groups[-1])
    with jax.named_scope("other_last"):
        attend_other(plan.groups[-1], 0)
        attend_other(plan.groups[-1], 1)
        for step in range(1, tp):
            for chunk in plan.groups[-1]:
                finish_other(step, chunk)

    with jax.named_scope("weight_wait"):
        tail_load.wait()
        if bits:
            for step in range(1, tp):
                for copy in level_copies(step, len(bits) - 1):
                    copy.wait_recv()

    wide = math.gcd(plan.out_columns, 768)

    def finish_rows(start, count):
        at = pl.ds(start, count)

        def own_columns(index):
            projected[at, lanes(t * plan.out_columns + index * wide, wide)] = jnp.dot(
                branch[at, :], own_out_weight[:, lanes(index * wide, wide)],
                preferred_element_type=f32,
            ).astype(bf16)

        pl.loop(0, plan.out_columns // wide)(own_columns)
        for step in range(1, tp):
            owner = lax.rem(t + tp - step, tp)

            def other_columns(index, step=step, owner=owner):
                projected[at, lanes(owner * plan.out_columns + index * wide, wide)] = jnp.dot(
                    branch[at, :], other_out_weight[step - 1, :, lanes(index * wide, wide)],
                    preferred_element_type=f32,
                ).astype(bf16)

            pl.loop(0, plan.out_columns // wide)(other_columns)
        block = math.gcd(count, 32)
        out_gain = sums[4:5, :] * post_gain_ref[...]

        def norm_block(index):
            here = pl.ds(pl.multiple_of(start + index * block, block), block)
            values = norm_rows(projected[here, :].astype(f32))
            out_ref[here, :] = (values * out_gain).astype(bf16)

        pl.loop(0, count // block)(norm_block)

    groups = [list(range(units - 1)), [units - 1]] if units > 1 else [[0]]
    for chunks in groups:
        with jax.named_scope("back_wait"):
            for chunk in chunks:
                for step in range(1, tp):
                    returned_here(step, chunk).wait_recv()
        with jax.named_scope("tail"):
            finish_rows(chunks[0] * unit, len(chunks) * unit)

    def scatter_done(index):
        copy, valid = scatter(index)
        only(every, valid, copy.wait_send)

    each(group - 1, scatter_done)
    only(
        every, me < plan.owners,
        lambda: each(group - 1, lambda index: gather(index).wait_send()),
    )
    for step in range(1, tp):
        kv_y(step).wait_send()
        for part in range(plan.parts):
            weight_y(step, part).wait_send()
        for turn in range(1, plan.pair):
            for part in range(plan.parts):
                weight_z(step, turn, part).wait_send()
        for chunk in range(units):
            row_copy(step, chunk).wait_send()
            returned(step, chunk).wait_send()
        for level in range(len(bits)):
            for copy in level_copies(step, level):
                copy.wait_send()
    for step in range(tp):
        for offset in range(1, sp):
            kv_z(step, offset).wait_send()


def mega(plan, lambdas, small, large):
    sp, tp, dp, group = plan.sp, plan.tp, plan.dp, plan.group
    rows, model, unit, units = plan.rows, plan.model, plan.unit, plan.units
    columns, stack = plan.columns, plan.stack
    others = max(tp - 1, 1)
    turns = max(plan.pair - 1, 1)
    swaps = max(dp - 1, 1)
    bf16, f32 = jnp.bfloat16, jnp.float32
    vmem = pl.BlockSpec(memory_space=pltpu.VMEM)
    dma = pltpu.SemaphoreType.DMA
    condition = small[0].shape[1]
    return pl.pallas_call(
        functools.partial(mega_kernel, plan),
        out_shape=jax.ShapeDtypeStruct((rows, model), bf16),
        in_specs=[pl.BlockSpec(memory_space=pltpu.SMEM)]
        + [vmem] * len(small)
        + [pl.BlockSpec(memory_space=pl.ANY)] * len(large),
        out_specs=vmem,
        scratch_shapes=[
            pltpu.VMEM((3, condition, model), bf16),
            pltpu.VMEM((rows, model), bf16),
            pltpu.VMEM((plan.context, model), bf16),
            pltpu.VMEM((plan.padded, model), bf16),
            pltpu.VMEM((model, KVH * 2 * LANES), bf16),
            pltpu.VMEM((model, columns), bf16),
            pltpu.VMEM((model, columns), bf16),
            pltpu.VMEM((plan.depth, plan.out_columns), bf16),
            pltpu.VMEM((others, plan.depth, plan.out_columns), bf16),
            pltpu.VMEM((others, rows, model), bf16),
            pltpu.VMEM((len(plan.groups[0]) * unit, model), bf16),
            pltpu.VMEM((KVH, plan.padded, 2 * LANES), bf16),
            pltpu.VMEM((group * plan.padded, 3 * LANES), bf16),
            pltpu.VMEM((8, model), f32),
            pltpu.VMEM((group - 1, 8, plan.slice), f32),
            pltpu.VMEM((8, model), f32),
            pltpu.VMEM((plan.padded, model), f32),
            pltpu.VMEM((tp * units, stack, LANES), bf16),
            pltpu.VMEM((tp * units, unit, columns), bf16),
            pltpu.VMEM((plan.half, max(plan.near, plan.far)), f32),
            pltpu.VMEM((plan.half, max(plan.near, plan.far)), f32),
            pltpu.VMEM((tp * units, stack, LANES), f32),
            pltpu.VMEM((tp * units, stack, LANES), f32),
            pltpu.VMEM((tp * units, stack, LANES), f32),
            pltpu.VMEM((rows, plan.depth), bf16),
            pltpu.VMEM((others, rows, columns), bf16),
            pltpu.VMEM((rows, model), bf16),
            dma((9 + 2 * KVH,)),
            dma((group - 1,)), dma((group - 1,)), dma((group - 1,)), dma((group - 1,)),
            dma((others, units)), dma((others, units)),
            dma((others,)), dma((others,)),
            dma((tp, sp - 1)), dma((tp, sp - 1)),
            dma((others, plan.parts)), dma((others, plan.parts)),
            dma((others, turns, plan.parts)), dma((others, turns, plan.parts)),
            dma((others, plan.pair, plan.parts)), dma((others, plan.pair, plan.parts)),
            dma((others, swaps)), dma((others, swaps)),
            dma((others, units)), dma((others, units)),
        ],
        compiler_params=pltpu.CompilerParams(
            collective_id=0, has_side_effects=True, vmem_limit_bytes=63 * 2**20
        ),
    )(lambdas, *small, *large)


def local(
    sp, tp, dp,
    latents, condition, context, context_cond,
    shift_weight, scale_weight, out_gate_weight,
    pre_gain, post_gain,
    query_weight, key_weight, value_weight, head_gate_weight,
    lambdas, head_gain, out_weight,
):
    plan = Plan(
        sp, tp, dp, latents.shape[1], context.shape[1], latents.shape[2],
        out_weight.shape, query_weight.shape[1],
    )
    result = mega(
        plan,
        lambdas,
        (
            condition, context_cond[None, :], pre_gain[None, :], post_gain[None, :],
            head_gain[None, :],
        ),
        (
            latents[0], context[0], shift_weight, scale_weight, out_gate_weight,
            query_weight, key_weight, value_weight, head_gate_weight, out_weight,
        ),
    )
    return result[None]


def solution(mesh):
    return jax.shard_map(
        functools.partial(local, mesh.shape["sp"], mesh.shape["tp"], mesh.shape["dp"]),
        mesh=mesh,
        in_specs=(
            P("dp", ("sp", "tp"), None),
            P("dp", ("sp", "tp")),
            P("dp", ("sp", "tp"), None),
            P(("sp", "tp")),
            P(("sp", "tp"), None),
            P(("sp", "tp"), None),
            P(("sp", "tp"), None),
            P(),
            P(),
            P(None, "tp"),
            P(),
            P(),
            P(None, "tp"),
            P("tp"),
            P(),
            P(None, "tp"),
        ),
        out_specs=P("dp", ("sp", "tp"), None),
        check_vma=False,
    )
```

```python
import functools
import math

import jax
import jax.numpy as jnp
from jax import lax
from jax.experimental import pallas as pl
from jax.experimental.pallas import tpu as pltpu
from jax.sharding import PartitionSpec as P

HEADS = 8
KVH = 2
HQK = 64
HV = 128
NORM_EPSILON = 1e-06
MESH = pl.DeviceIdType.MESH
SUBLANES = 16
LANES = 128


def norm_rows(values):
    return values * lax.rsqrt(jnp.mean(values * values, axis=-1, keepdims=True) + NORM_EPSILON)


def each(count, body):
    if count <= 8:
        for index in range(count):
            body(index)
    else:
        pl.loop(0, count)(body)


def only(always, condition, body):
    if always:
        body()
    else:
        pl.when(condition)(body)


def flip(index, bit):
    return index + bit - 2 * bit * lax.rem(index // bit, 2)


def lanes(start, size):
    return pl.ds(pl.multiple_of(start, LANES), size)


def rows_at(start, size):
    return pl.ds(pl.multiple_of(start, math.gcd(size, SUBLANES)), size)


class Plan:
    def __init__(self, sp, tp, dp, rows, context, model, weight_shape, query_columns):
        self.sp, self.tp, self.dp = sp, tp, dp
        self.group = sp * tp
        self.rows, self.context, self.model = rows, context, model
        self.columns = query_columns
        self.local_heads = query_columns // (2 * HQK)
        self.per_group = (HEADS // KVH) // self.local_heads
        self.used = rows + context
        self.padded = -(-self.used // SUBLANES) * SUBLANES
        self.owners = math.gcd(model // LANES, self.group)
        self.slice = model // self.owners
        self.depth, self.out_columns = weight_shape
        self.quarter = self.depth // dp
        self.pair = math.gcd(math.gcd(sp, 2), self.quarter // SUBLANES)
        self.share = self.quarter // self.pair
        self.parts = math.gcd(4, self.share // SUBLANES)
        self.unit = max(SUBLANES, rows // 4 // SUBLANES * SUBLANES)
        self.units = rows // self.unit
        self.stack = self.local_heads * 2 * self.unit
        self.half = self.stack // 2
        first = [(0, self.unit)]
        if self.unit > SUBLANES:
            cut = self.unit // 2 // SUBLANES * SUBLANES
            first = [(0, cut), (cut, self.unit - cut)]
        self.pieces = first + [(chunk * self.unit, self.unit) for chunk in range(1, self.units)]
        self.chunk_pieces = [list(range(len(first)))] + [
            [len(first) + chunk] for chunk in range(self.units - 1)
        ]
        self.near = (tp + sp - 1) * self.padded
        self.far = (tp - 1) * (sp - 1) * self.padded
        self.groups = [[0]] + [[chunk] for chunk in range(1, self.units)]
        if self.units > 2:
            self.groups = [[0, 1]] + [[chunk] for chunk in range(2, self.units)]


def modulate_rows(source, target, start, count, target_start, gain_scale, shift):
    block = math.gcd(count, 32)

    def step(index):
        offset = pl.multiple_of(index * block, block)
        values = norm_rows(source[pl.ds(start + offset, block), :].astype(jnp.float32))
        result = values * gain_scale + shift
        target[pl.ds(target_start + offset, block), :] = result.astype(jnp.bfloat16)

    pl.loop(0, count // block)(step)


def mega_kernel(
    plan,
    lambda_ref, cond_ref, context_cond_ref, gain_ref, post_gain_ref, head_gain_ref,
    latents, context, shift_weight, scale_weight, gate_weight,
    query_weight, key_weight, value_weight, head_gate_weight, out_weight,
    out_ref,
    wcond, own_rows, own_context, own_in, kv_weight, q_weight, g_weight, own_out_weight,
    other_out_weight, other_rows, other_in, kv_made, kv, parts, held, sums, normed,
    queries, gates, scores_a, scores_b, weighted, normalizer, largest, branch, back, projected,
    load_sem, sum_send, sum_recv, all_send, all_recv,
    row_send, row_recv, kvy_send, kvy_recv, kvz_send, kvz_recv,
    wy_send, wy_recv, wz_send, wz_recv, wx_send, wx_recv, wd_send, wd_recv,
    back_send, back_recv,
):
    sp, tp, dp, group = plan.sp, plan.tp, plan.dp, plan.group
    s, t, d = lax.axis_index("sp"), lax.axis_index("tp"), lax.axis_index("dp")
    me = s * tp + t
    rows, context_rows, unit, units = plan.rows, plan.context, plan.unit, plan.units
    heads, columns, size = plan.local_heads, plan.columns, plan.padded
    f32, bf16 = jnp.float32, jnp.bfloat16

    def load(index, source, target):
        copy = pltpu.make_async_copy(source, target, load_sem.at[index])
        copy.start()
        return copy

    cond_loads = [
        load(i, w, wcond.at[i]) for i, w in enumerate((shift_weight, scale_weight, gate_weight))
    ]
    row_load = load(3, latents, own_rows)
    context_load = load(4, context, own_context)
    def member(offset):
        other = lax.rem(me + offset, group)
        return {"sp": other // tp, "tp": lax.rem(other, tp)}

    def remote(source, target, send, recv, device):
        return pltpu.make_async_remote_copy(
            src_ref=source, dst_ref=target, send_sem=send, recv_sem=recv,
            device_id=device, device_id_type=MESH,
        )

    bits = []
    bit = dp // 2
    while bit:
        bits.append(bit)
        bit //= 2

    barrier = pltpu.get_barrier_semaphore()

    def greet(index):
        pl.semaphore_signal(
            barrier, inc=1, device_id=member(index + 1), device_id_type=MESH
        )

    each(group - 1, greet)
    for bit in bits:
        pl.semaphore_signal(
            barrier, inc=1, device_id={"dp": flip(d, bit)}, device_id_type=MESH
        )

    base = s - lax.rem(s, plan.pair)
    ring = lax.rem(s, plan.pair)
    piece = plan.share // plan.parts

    def over_tp(step):
        return {"tp": lax.rem(t + step, tp)}

    def weight_y(step, part):
        at = rows_at((d * plan.pair + ring) * plan.share + part * piece, piece)
        return remote(
            out_weight.at[at, :], other_out_weight.at[step - 1, at, :],
            wy_send.at[step - 1, part], wy_recv.at[step - 1, part], over_tp(step),
        )

    def weight_z(step, turn, part):
        at = rows_at((d * plan.pair + ring) * plan.share + part * piece, piece)
        return remote(
            other_out_weight.at[step - 1, at, :], other_out_weight.at[step - 1, at, :],
            wz_send.at[step - 1, turn - 1, part], wz_recv.at[step - 1, turn - 1, part],
            {"sp": base + lax.rem(ring + turn, plan.pair)},
        )

    def weight_x(step, turn, part):
        source = lax.rem(ring + turn, plan.pair)
        at = rows_at((d * plan.pair + source) * plan.share + part * piece, piece)
        return remote(
            other_out_weight.at[step - 1, at, :], other_out_weight.at[step - 1, at, :],
            wx_send.at[step - 1, turn, part], wx_recv.at[step - 1, turn, part],
            {"dp": flip(d, bits[0])},
        )

    def weight_d(step, level, index):
        turns = [0]
        for earlier in bits[:level]:
            turns += [turn ^ earlier for turn in turns]
        source = d
        for other in bits:
            if turns[index] & other:
                source = flip(source, other)
        at = rows_at(source * plan.quarter, plan.quarter)
        slot = (2**level - 1) + index
        return remote(
            other_out_weight.at[step - 1, at, :], other_out_weight.at[step - 1, at, :],
            wd_send.at[step - 1, slot], wd_recv.at[step - 1, slot],
            {"dp": flip(d, bits[level])},
        )

    def level_copies(step, level):
        if level == 0:
            return [
                weight_x(step, turn, part)
                for turn in range(plan.pair) for part in range(plan.parts)
            ]
        return [weight_d(step, level, index) for index in range(2**level)]

    def row_copy(step, number):
        at = pl.ds(*plan.pieces[number])
        return remote(
            latents.at[at, :], other_rows.at[step - 1, at, :],
            row_send.at[step - 1, number], row_recv.at[step - 1, number], over_tp(step),
        )

    def over_tp_steps(body):
        if tp <= 3:
            for step in range(1, tp):
                body(step)
        else:
            pl.loop(1, tp)(body)

    with jax.named_scope("enter"):
        pl.semaphore_wait(barrier, group - 1 + len(bits))

    def weight_start(part):
        if part < plan.parts:
            over_tp_steps(lambda step: weight_y(step, part).start())

    def weight_forward(part):
        if part < plan.parts:
            for step in range(1, tp):
                weight_y(step, part).wait_recv()
                if bits:
                    weight_x(step, 0, part).start()
                for turn in range(1, plan.pair):
                    weight_z(step, turn, part).start()

    def weight_pair(part):
        if part < plan.parts:
            with jax.named_scope("weight_pair"):
                for step in range(1, tp):
                    for turn in range(1, plan.pair):
                        weight_z(step, turn, part).wait_recv()
                        if bits:
                            weight_x(step, turn, part).start()

    weight_start(0)

    with jax.named_scope("conditions"):
        conditions = []
        for ref in (cond_ref, context_cond_ref):
            value = ref[...].astype(f32)
            value = value / (1.0 + jnp.exp(-value))
            conditions.append(value.reshape(1, value.shape[-1]))
        depth = cond_ref.shape[1]
        index = lax.broadcasted_iota(jnp.int32, (8, depth), 0)
        first = jnp.broadcast_to(conditions[0], (8, depth))
        second = jnp.broadcast_to(conditions[1], (8, depth))
        lefts = []
        for number in range(3):
            left = jnp.where(index == 2 * number, first, 0.0)
            if number < 2:
                left = jnp.where(index == 2 * number + 1, second, left)
            lefts.append(left.astype(bf16))
        width = plan.slice
        for copy in cond_loads:
            copy.wait()
        kv_loads = []
        for head in range(KVH):
            for part, weight in enumerate((key_weight, value_weight)):
                kv_loads.append(
                    load(
                        5 + 2 * head + part,
                        weight.at[:, pl.ds(head * LANES, LANES)],
                        kv_weight.at[:, pl.ds((2 * head + part) * LANES, LANES)],
                    )
                )
        late_loads = [
            load(5 + 2 * KVH, query_weight, q_weight),
            load(6 + 2 * KVH, head_gate_weight, g_weight),
        ]
        tail_load = load(7 + 2 * KVH, out_weight, own_out_weight)

        def partial_sums(column):
            at = lanes(column * width, width)
            total = None
            for number in range(3):
                part = jnp.dot(lefts[number], wcond[number, :, at], preferred_element_type=f32)
                total = part if total is None else total + part
            parts[:, at] = total

        each(plan.owners, partial_sums)

    every = plan.owners == group

    def scatter(index):
        owner = lax.rem(me + index + 1, group)
        return remote(
            parts.at[:, lanes(lax.rem(owner, plan.owners) * width, width)],
            held.at[index], sum_send.at[index], sum_recv.at[index], member(index + 1),
        ), owner < plan.owners

    def scatter_start(index):
        copy, valid = scatter(index)
        only(every, valid, copy.start)

    each(group - 1, scatter_start)

    weight_start(1)
    row_load.wait()
    block = math.gcd(rows, 32)

    def normalize(index):
        at = pl.ds(pl.multiple_of(index * block, block), block)
        normed[at, :] = norm_rows(own_rows[at, :].astype(f32))

    with jax.named_scope("normalize"):
        pl.loop(0, rows // block)(normalize)
        context_load.wait()
        normed[rows : rows + context_rows, :] = norm_rows(own_context[...].astype(f32))

    own_slice = lanes(lax.rem(me, plan.owners) * width, width)

    def gather(index):
        return remote(
            sums.at[:, own_slice], sums.at[:, own_slice],
            all_send.at[index], all_recv.at[index], member(index + 1),
        )

    def arrived(index):
        origin = lax.rem(me + group - index - 1, group)
        at = lanes(lax.rem(origin, plan.owners) * width, width)
        return remote(
            sums.at[:, at], sums.at[:, at],
            all_send.at[index], all_recv.at[index], member(index + 1),
        ), origin < plan.owners

    def own_sum():
        each(group - 1, lambda index: scatter(index)[0].wait_recv())
        total = parts[:, own_slice]
        if group <= 16:
            for index in range(group - 1):
                total = total + held[index]
        else:
            total = lax.fori_loop(
                0, group - 1, lambda index, value: value + held[index], total
            )
        sums[:, own_slice] = total
        each(group - 1, lambda index: gather(index).start())

    with jax.named_scope("reduce"):
        only(every, me < plan.owners, own_sum)

    weight_start(2)
    over_tp_steps(lambda step: row_copy(step, 0).start())
    kv[:, 2 * LANES :] = jnp.ones((kv.shape[0], LANES), bf16)

    def sum_arrival(index):
        copy, valid = arrived(index)
        only(every, valid, copy.wait_recv)

    with jax.named_scope("gather"):
        each(group - 1, sum_arrival)
    with jax.named_scope("weight_forward"):
        weight_forward(0)
        weight_forward(1)
    gain = gain_ref[...]
    shift, context_shift = sums[0:1, :], sums[1:2, :]
    gain_scale, context_gain_scale = gain * (1.0 + sums[2:3, :]), gain * (1.0 + sums[3:4, :])
    with jax.named_scope("modulate"):

        def modulate(index):
            at = pl.ds(pl.multiple_of(index * block, block), block)
            own_in[at, :] = (normed[at, :] * gain_scale + shift).astype(bf16)

        pl.loop(0, rows // block)(modulate)
        values = normed[rows : rows + context_rows, :] * context_gain_scale + context_shift
        if size > plan.used:
            fill = jnp.zeros((size - plan.used, plan.model), f32)
            values = jnp.concatenate([values, fill], axis=0)
        own_in[rows:, :] = values.astype(bf16)
    for copy in kv_loads:
        copy.wait()

    def make_kv(head):
        kv_made[head] = jnp.dot(
            own_in[...], kv_weight[:, lanes(head * 2 * LANES, 2 * LANES)],
            preferred_element_type=f32,
        ).astype(bf16)

    with jax.named_scope("make_kv"):
        pl.loop(0, KVH)(make_kv)

    def kv_slot(step, offset):
        slot = step if offset == 0 else tp + step * (sp - 1) + offset - 1
        return kv.at[pl.ds(slot * size, size), pl.ds(0, 2 * LANES)]

    def kv_group(column):
        return column // plan.per_group

    def kv_y(step):
        return remote(
            kv_made.at[kv_group(lax.rem(t + step, tp))], kv_slot(step, 0),
            kvy_send.at[step - 1], kvy_recv.at[step - 1], over_tp(step),
        )

    def kv_z(step, offset):
        source = kv_made.at[kv_group(t)] if step == 0 else kv_slot(step, 0)
        return remote(
            source, kv_slot(step, offset),
            kvz_send.at[step, offset - 1], kvz_recv.at[step, offset - 1],
            {"sp": lax.rem(s + offset, sp)},
        )

    over_tp_steps(lambda step: kv_y(step).start())
    own_block = load(8 + 2 * KVH, kv_made.at[kv_group(t)], kv_slot(0, 0))
    for offset in range(1, sp):
        kv_z(0, offset).start()
    for number in range(1, len(plan.pieces)):
        if number + 1 == len(plan.pieces):
            weight_start(3)
        over_tp_steps(lambda step, number=number: row_copy(step, number).start())
    if len(plan.pieces) == 1:
        weight_start(3)

    def project_rows(source, start, count, first_unit):
        wide = math.gcd(columns, 512)

        def make_queries(index):
            result = jnp.dot(
                source[pl.ds(start, count), :], q_weight[:, lanes(index * wide, wide)],
                preferred_element_type=f32,
            ).astype(bf16).astype(f32) * HQK ** (-0.5)
            lane = lax.broadcasted_iota(jnp.int32, (count, LANES), 1)
            for local in range(wide // LANES):
                value = result[:, local * LANES : (local + 1) * LANES]
                head = index * (wide // LANES) + local
                for number in range(2):
                    half = jnp.where((lane < HQK) == (number == 0), value, 0.0).astype(bf16)
                    for block in range(count // unit):
                        at = rows_at((head * 2 + number) * unit, unit)
                        queries[first_unit + block, at, :] = half[
                            block * unit : (block + 1) * unit
                        ]

        def make_gates(index):
            at = lanes(index * wide, wide)
            result = jnp.dot(
                source[pl.ds(start, count), :], g_weight[:, at], preferred_element_type=f32
            ).astype(bf16)
            for block in range(count // unit):
                gates[first_unit + block, :, at] = result[block * unit : (block + 1) * unit]

        pl.loop(0, columns // wide)(make_queries)
        pl.loop(0, columns // wide)(make_gates)

    for copy in late_loads:
        copy.wait()
    with jax.named_scope("own_project"):
        project_rows(own_in, 0, rows, 0)

    with jax.named_scope("kv_over_tp"):
        for step in range(1, tp):
            kv_y(step).wait_recv()

    def forward():
        for step in range(1, tp):
            for offset in range(1, sp):
                kv_z(step, offset).start()

    contract = (((1,), (1,)), ((), ()))

    here = tp * size
    spans = {
        "here": (0, here), "middle": (here, plan.near - here),
        "near": (0, plan.near), "far": (plan.near, plan.far),
    }

    def follows(phase):
        return phase in ("middle", "far")

    def score(buffer, index, side, phase):
        begin, count = spans[phase]
        result = lax.dot_general(
            queries[index, pl.ds(side * plan.half, plan.half), :],
            kv[pl.ds(begin, count), pl.ds(0, LANES)],
            contract, preferred_element_type=f32,
        )
        if plan.used < size:
            column = lax.broadcasted_iota(jnp.int32, result.shape, 1)
            result = jnp.where(lax.rem(column, size) < plan.used, result, -jnp.inf)
        buffer[:, pl.ds(0, count)] = result

    def gather_values(buffer, index, side, phase):
        begin, count = spans[phase]
        at = pl.ds(side * plan.half, plan.half)
        scores = buffer[:, pl.ds(0, count)]
        top = jnp.max(scores, axis=-1, keepdims=True)
        if follows(phase):
            before = largest[index, at, pl.ds(0, 1)]
            top = jnp.maximum(top, before)
        both = jnp.dot(
            jnp.exp(scores - top).astype(bf16), kv[pl.ds(begin, count), pl.ds(LANES, 2 * LANES)],
            preferred_element_type=f32,
        )
        if follows(phase):
            keep = jnp.exp(before - top)
            weighted[index, at, :] = weighted[index, at, :] * keep + both[:, :LANES]
            normalizer[index, at, :] = normalizer[index, at, :] * keep + both[:, LANES:]
        else:
            weighted[index, at, :] = both[:, :LANES]
            normalizer[index, at, :] = both[:, LANES:]
        if phase != "far":
            largest[index, at, :] = jnp.broadcast_to(top, (plan.half, LANES))

    def attend(first_unit, count, phase):
        if not spans[phase][1]:
            return
        score(scores_a, first_unit, 0, phase)

        def step(index):
            here = first_unit + index
            score(scores_b, here, 1, phase)
            gather_values(scores_a, here, 0, phase)
            score(scores_a, here + 1, 0, phase)
            gather_values(scores_b, here, 1, phase)

        if count > 1:
            pl.loop(0, count - 1)(step)
        score(scores_b, first_unit + count - 1, 1, phase)
        gather_values(scores_a, first_unit + count - 1, 0, phase)
        gather_values(scores_b, first_unit + count - 1, 1, phase)

    def finish(index, target):
        for head in range(heads):
            ratios = []
            for number in range(2):
                at = pl.ds((head * 2 + number) * unit, unit)
                ratios.append(weighted[index, at, :] / normalizer[index, at, :])
            attended = ratios[0] - lambda_ref[head] * ratios[1]
            gate = gates[index, :, pl.ds(head * LANES, LANES)].astype(f32)
            gate = gate / (1.0 + jnp.exp(-gate))
            target(head, (norm_rows(attended) * head_gain_ref[...] * gate).astype(bf16))

    def finish_own(index):
        at = rows_at(index * unit, unit)

        def store(head, value):
            branch[at, lanes(t * columns + head * LANES, LANES)] = value

        finish(index, store)

    def returned(step, chunk):
        at = pl.ds(chunk * unit, unit)
        return remote(
            back.at[step - 1, at, :], branch.at[at, lanes(t * columns, columns)],
            back_send.at[step - 1, chunk], back_recv.at[step - 1, chunk],
            over_tp(tp - step),
        )

    def returned_here(step, chunk):
        owner = lax.rem(t + step, tp)
        at = pl.ds(chunk * unit, unit)
        return remote(
            back.at[step - 1, at, :], branch.at[at, lanes(owner * columns, columns)],
            back_send.at[step - 1, chunk], back_recv.at[step - 1, chunk],
            over_tp(tp - step),
        )

    def finish_other(step, chunk):
        def store(head, value):
            back[step - 1, pl.ds(chunk * unit, unit), pl.ds(head * LANES, LANES)] = value

        finish(step * units + chunk, store)
        returned(step, chunk).start()

    def receive(chunks):
        begin, count = chunks[0] * unit, len(chunks) * unit

        def one(step):
            with jax.named_scope("row_wait"):
                for chunk in chunks:
                    for number in plan.chunk_pieces[chunk]:
                        row_copy(step, number).wait_recv()
            with jax.named_scope("other_project"):
                modulate_rows(other_rows.at[step - 1], other_in, begin, count, 0, gain_scale, shift)
                project_rows(other_in, 0, count, step * units + chunks[0])

        over_tp_steps(one)

    def attend_other(chunks, phase):
        over_tp_steps(lambda step: attend(step * units + chunks[0], len(chunks), phase))

    def finish_others(chunks):
        def one(step):
            for chunk in chunks:
                finish_other(step, chunk)

        over_tp_steps(one)

    def kv_wait(step):
        with jax.named_scope("kv_wait"):
            for offset in range(1, sp):
                kv_z(step, offset).wait_recv()

    own_block.wait()
    with jax.named_scope("own_here"):
        attend(0, units, "here")
    forward()
    weight_forward(2)
    weight_pair(0)
    weight_pair(1)
    kv_wait(0)
    with jax.named_scope("own_middle"):
        attend(0, units, "middle")
    for number, chunks in enumerate(plan.groups[:-1]):
        receive(chunks)
        with jax.named_scope("other_near"):
            attend_other(chunks, "near")
        if number == 0:
            weight_pair(2)
    if len(plan.groups) == 1:
        weight_pair(2)
    def weight_levels():
        for level in range(len(bits) - 1):
            with jax.named_scope("weight_dp"):
                for step in range(1, tp):
                    for copy in level_copies(step, level):
                        copy.wait_recv()
                    for copy in level_copies(step, level + 1):
                        copy.start()

    for step in range(1, tp):
        kv_wait(step)
    early = [chunk for chunks in plan.groups[:-1] for chunk in chunks]
    if early:
        with jax.named_scope("other_far"):
            attend_other(early, "far")
            finish_others(early)
    weight_forward(3)
    with jax.named_scope("own_far"):
        attend(0, units, "far")
        pl.loop(0, units)(finish_own)
    weight_pair(3)
    receive(plan.groups[-1])
    with jax.named_scope("other_last"):
        attend_other(plan.groups[-1], "near")
        attend_other(plan.groups[-1], "far")
        finish_others(plan.groups[-1])

    def weights_here():
        with jax.named_scope("weight_wait"):
            if bits:
                for step in range(1, tp):
                    for copy in level_copies(step, len(bits) - 1):
                        copy.wait_recv()

    tail_load.wait()
    weight_levels()
    wide = math.gcd(plan.out_columns, 768)

    def own_projection(at):
        def own_columns(index):
            projected[at, lanes(t * plan.out_columns + index * wide, wide)] = jnp.dot(
                branch[at, :], own_out_weight[:, lanes(index * wide, wide)],
                preferred_element_type=f32,
            ).astype(bf16)

        pl.loop(0, plan.out_columns // wide)(own_columns)

    def other_projection(at):
        def one(step):
            owner = lax.rem(t + tp - step, tp)

            def other_columns(index):
                projected[at, lanes(owner * plan.out_columns + index * wide, wide)] = jnp.dot(
                    branch[at, :], other_out_weight[step - 1, :, lanes(index * wide, wide)],
                    preferred_element_type=f32,
                ).astype(bf16)

            pl.loop(0, plan.out_columns // wide)(other_columns)

        over_tp_steps(one)

    def scale_out(start, count):
        block = math.gcd(count, 32)
        out_gain = sums[4:5, :] * post_gain_ref[...]

        def one(index):
            here = pl.ds(pl.multiple_of(start + index * block, block), block)
            values = norm_rows(projected[here, :].astype(f32))
            projected[here, :] = (values * out_gain).astype(bf16)

        pl.loop(0, count // block)(one)

    stores = []
    groups = [list(range(units - 1)), [units - 1]] if units > 1 else [[0]]
    for chunks in groups:
        with jax.named_scope("back_wait"):
            for chunk in chunks:
                for step in range(1, tp):
                    returned_here(step, chunk).wait_recv()
        at = pl.ds(chunks[0] * unit, len(chunks) * unit)
        with jax.named_scope("tail"):
            own_projection(at)
        if chunks is groups[0]:
            weights_here()
        with jax.named_scope("tail"):
            other_projection(at)
        with jax.named_scope("out_norm"):
            scale_out(chunks[0] * unit, len(chunks) * unit)
            stores.append(
                load(9 + 2 * KVH + len(stores), projected.at[at, :], out_ref.at[at, :])
            )

    def scatter_done(index):
        copy, valid = scatter(index)
        only(every, valid, copy.wait_send)

    each(group - 1, scatter_done)
    for store in stores:
        store.wait()
    only(
        every, me < plan.owners,
        lambda: each(group - 1, lambda index: gather(index).wait_send()),
    )
    for step in range(1, tp):
        kv_y(step).wait_send()
        for part in range(plan.parts):
            weight_y(step, part).wait_send()
        for turn in range(1, plan.pair):
            for part in range(plan.parts):
                weight_z(step, turn, part).wait_send()
        for number in range(len(plan.pieces)):
            row_copy(step, number).wait_send()
        for chunk in range(units):
            returned(step, chunk).wait_send()
        for level in range(len(bits)):
            for copy in level_copies(step, level):
                copy.wait_send()
    for step in range(tp):
        for offset in range(1, sp):
            kv_z(step, offset).wait_send()


def mega(plan, lambdas, small, large):
    sp, tp, dp, group = plan.sp, plan.tp, plan.dp, plan.group
    rows, model, unit, units = plan.rows, plan.model, plan.unit, plan.units
    columns, stack = plan.columns, plan.stack
    others = max(tp - 1, 1)
    turns = max(plan.pair - 1, 1)
    swaps = max(dp - 1, 1)
    bf16, f32 = jnp.bfloat16, jnp.float32
    vmem = pl.BlockSpec(memory_space=pltpu.VMEM)
    dma = pltpu.SemaphoreType.DMA
    condition = small[0].shape[1]
    return pl.pallas_call(
        functools.partial(mega_kernel, plan),
        out_shape=jax.ShapeDtypeStruct((rows, model), bf16),
        in_specs=[pl.BlockSpec(memory_space=pltpu.SMEM)]
        + [vmem] * len(small)
        + [pl.BlockSpec(memory_space=pl.ANY)] * len(large),
        out_specs=pl.BlockSpec(memory_space=pl.ANY),
        scratch_shapes=[
            pltpu.VMEM((3, condition, model), bf16),
            pltpu.VMEM((rows, model), bf16),
            pltpu.VMEM((plan.context, model), bf16),
            pltpu.VMEM((plan.padded, model), bf16),
            pltpu.VMEM((model, KVH * 2 * LANES), bf16),
            pltpu.VMEM((model, columns), bf16),
            pltpu.VMEM((model, columns), bf16),
            pltpu.VMEM((plan.depth, plan.out_columns), bf16),
            pltpu.VMEM((others, plan.depth, plan.out_columns), bf16),
            pltpu.VMEM((others, rows, model), bf16),
            pltpu.VMEM((len(plan.groups[0]) * unit, model), bf16),
            pltpu.VMEM((KVH, plan.padded, 2 * LANES), bf16),
            pltpu.VMEM((group * plan.padded, 3 * LANES), bf16),
            pltpu.VMEM((8, model), f32),
            pltpu.VMEM((group - 1, 8, plan.slice), f32),
            pltpu.VMEM((8, model), f32),
            pltpu.VMEM((plan.padded, model), f32),
            pltpu.VMEM((tp * units, stack, LANES), bf16),
            pltpu.VMEM((tp * units, unit, columns), bf16),
            pltpu.VMEM((plan.half, max(plan.near, plan.far)), f32),
            pltpu.VMEM((plan.half, max(plan.near, plan.far)), f32),
            pltpu.VMEM((tp * units, stack, LANES), f32),
            pltpu.VMEM((tp * units, stack, LANES), f32),
            pltpu.VMEM((tp * units, stack, LANES), f32),
            pltpu.VMEM((rows, plan.depth), bf16),
            pltpu.VMEM((others, rows, columns), bf16),
            pltpu.VMEM((rows, model), bf16),
            dma((11 + 2 * KVH,)),
            dma((group - 1,)), dma((group - 1,)), dma((group - 1,)), dma((group - 1,)),
            dma((others, units + 1)), dma((others, units + 1)),
            dma((others,)), dma((others,)),
            dma((tp, sp - 1)), dma((tp, sp - 1)),
            dma((others, plan.parts)), dma((others, plan.parts)),
            dma((others, turns, plan.parts)), dma((others, turns, plan.parts)),
            dma((others, plan.pair, plan.parts)), dma((others, plan.pair, plan.parts)),
            dma((others, swaps)), dma((others, swaps)),
            dma((others, units)), dma((others, units)),
        ],
        compiler_params=pltpu.CompilerParams(
            collective_id=0, has_side_effects=True, vmem_limit_bytes=63 * 2**20
        ),
    )(lambdas, *small, *large)


def local(
    sp, tp, dp,
    latents, condition, context, context_cond,
    shift_weight, scale_weight, out_gate_weight,
    pre_gain, post_gain,
    query_weight, key_weight, value_weight, head_gate_weight,
    lambdas, head_gain, out_weight,
):
    plan = Plan(
        sp, tp, dp, latents.shape[1], context.shape[1], latents.shape[2],
        out_weight.shape, query_weight.shape[1],
    )
    result = mega(
        plan,
        lambdas,
        (
            condition, context_cond, pre_gain[None, :], post_gain[None, :],
            head_gain[None, :],
        ),
        (
            latents[0], context[0], shift_weight, scale_weight, out_gate_weight,
            query_weight, key_weight, value_weight, head_gate_weight, out_weight,
        ),
    )
    return result[None]


def solution(mesh):
    return jax.shard_map(
        functools.partial(local, mesh.shape["sp"], mesh.shape["tp"], mesh.shape["dp"]),
        mesh=mesh,
        in_specs=(
            P("dp", ("sp", "tp"), None),
            P("dp", ("sp", "tp")),
            P("dp", ("sp", "tp"), None),
            P(("sp", "tp")),
            P(("sp", "tp"), None),
            P(("sp", "tp"), None),
            P(("sp", "tp"), None),
            P(),
            P(),
            P(None, "tp"),
            P(),
            P(),
            P(None, "tp"),
            P("tp"),
            P(),
            P(None, "tp"),
        ),
        out_specs=P("dp", ("sp", "tp"), None),
        check_vma=False,
    )
```
